32 devices in a mesh: kv: 8 (over z, y), tp: 4 (over x, core).
Axes of the slice: x: 2, y: 2, z: 4, core: 2. Of those that a mesh axis runs over, the one named last changes fastest.
Arguments:
- tokens: bfloat16 [2048, 4096], P('kv'), may hold values from -6 to 6
- norm_gain: float32 [4096], replicated, may hold values from 0.1 to 1.9
- w_query: bfloat16 [4096, 2048], P('kv', 'tp'), may hold values from -0.09375 to 0.09375
- w_forget: bfloat16 [4096, 2048], P('kv', 'tp'), may hold values from -0.09375 to 0.09375
- w_value: bfloat16 [4096, 2048], P('kv', 'tp'), may hold values from -0.09375 to 0.09375
- w_gate: bfloat16 [4096, 2048], P('kv', 'tp'), may hold values from -0.09375 to 0.09375
- lower_bound: float32 [2048], P('tp'), may hold values from 0 to 0.9
- head_gain: float32 [2048], P('tp'), may hold values from 0.1 to 1.9
- w_out: bfloat16 [2048, 4096], P('kv', 'tp'), may hold values from -0.125 to 0.125
- state: float32 [512, 16, 128, 128], P('kv', 'tp'), may hold values from -4 to 4
- prev_forget: bfloat16 [512, 4, 2048], P('kv', None, 'tp'), may hold values from -8 to 8
- prev_value: bfloat16 [512, 4, 2048], P('kv', None, 'tp'), may hold values from -6 to 6
- accepted: int32 [512], P('kv'), may hold values from 0 to 4
Outputs:
- mixed: bfloat16 [2048, 4096], P('kv', 'tp')
- taken_state: float32 [512, 16, 128, 128], P('kv', 'tp')
The draws below stay inside these ranges and needn't reach their ends.
All inputs are finite; a program needn't handle non-finite values.
Results may differ from the reference program's by a relative error of at most 0.015.
Values may be sent and summed in bfloat16 or wider, within the bound.
A program may use at most 128 MiB of HBM per device.

```python
import jax
import jax.numpy as jnp
from jax import lax

D = 4096
HEADS = 16
KEY_DIM = 128
VAL_DIM = 128
PROPOSALS = 4
SEQS = 512
TOKENS = 2048
WIDTH = 2048


def with_ends(entries, own_key, least, largest):
    longest = entries.shape.index(max(entries.shape))
    spots = []
    for shift in (0, 1):
        where = [jax.random.randint(jax.random.fold_in(own_key, axis), (), 0, length) for axis, length in enumerate(entries.shape)]
        where[longest] = (where[longest] + shift) % entries.shape[longest]
        spots.append(tuple(where))
    return entries.at[spots[0]].set(least).at[spots[1]].set(largest)


def steps_of(own_key, extent, split, smallest, top_value):
    loudness, own = 1.0, jax.random.fold_in(own_key, 6)
    for axis_at, shards_of in split:
        heights = jnp.exp(jax.random.uniform(jax.random.fold_in(own, axis_at), (shards_of,), jnp.float32, smallest / len(split), top_value / len(split)))
        loudness = loudness * jnp.repeat(heights, extent[axis_at] // shards_of).reshape([-1 if axis == axis_at else 1 for axis in range(len(extent))])
    return loudness


def bell_draw(key, shape, width, reach, shards=(), kind=jnp.bfloat16):
    loudness = steps_of(key, shape, shards, -0.22, 0.18) if shards else 1.0
    result = jax.random.normal(key, shape, jnp.float32) * width * loudness
    return jnp.minimum(jnp.maximum(result, -reach), reach).astype(kind)


def setup_inputs(seed: int = 0) -> dict:
    key_of = jax.random.split(jax.random.key(seed), 14)
    return {
        "tokens": bell_draw(key_of[0], (TOKENS, D), 1.0, 6.0, ((0, 8),)),
        "norm_gain": jnp.clip(1.0 + 0.18 * jax.random.normal(key_of[1], (D,), jnp.float32), 0.1, 1.9),
        "w_query": bell_draw(key_of[2], (D, WIDTH), D ** -0.5, 0.09375, ((0, 8), (1, 4))),
        "w_forget": bell_draw(key_of[3], (D, WIDTH), D ** -0.5, 0.09375, ((0, 8), (1, 4))),
        "w_value": bell_draw(key_of[4], (D, WIDTH), D ** -0.5, 0.09375, ((0, 8), (1, 4))),
        "w_gate": bell_draw(key_of[5], (D, WIDTH), D ** -0.5, 0.09375, ((0, 8), (1, 4))),
        "lower_bound": jnp.clip(0.9 * jax.random.uniform(key_of[6], (WIDTH,), jnp.float32) ** steps_of(key_of[6], (WIDTH,), ((0, 4),), -0.2, 0.2), 0.0, 0.9),
        "head_gain": jnp.clip(1.0 + 0.18 * jax.random.normal(key_of[7], (WIDTH,), jnp.float32), 0.1, 1.9),
        "w_out": bell_draw(key_of[8], (WIDTH, D), WIDTH ** -0.5, 0.125, ((0, 8), (1, 4))),
        "state": bell_draw(key_of[9], (SEQS, HEADS, KEY_DIM, VAL_DIM), 0.5, 4.0, ((0, 8), (1, 4)), jnp.float32),
        "prev_forget": bell_draw(key_of[10], (SEQS, PROPOSALS, WIDTH), 1.5, 8.0, ((0, 8), (2, 4))),
        "prev_value": bell_draw(key_of[11], (SEQS, PROPOSALS, WIDTH), 1.0, 6.0, ((0, 8), (2, 4))),
        "accepted": with_ends(jax.random.randint(key_of[12], (SEQS,), 0, PROPOSALS + 1), jax.random.fold_in(key_of[12], 1), 0, PROPOSALS).astype(jnp.int32),
    }


EPSILON = 1e-06

def forget_of(pre_act, bounds):
    return bounds + (1.0 - bounds) * jax.nn.sigmoid(pre_act.astype(jnp.float32))

def recur_one(start_state, old_forget, old_values, accepted_count, queries, forget, new_values):
    carried = start_state
    for position in range(old_forget.shape[0]):
        kept_mask = position < accepted_count
        decay_rate = jnp.where(kept_mask, old_forget[position], 1.0)
        weight = jnp.where(kept_mask, 1.0 - old_forget[position], 0.0)
        carried = decay_rate[:, :, None] * carried + weight[:, :, None] * old_values[position][:, None, :]
    taken = carried
    outputs = []
    for position in range(queries.shape[0]):
        carried = forget[position][:, :, None] * carried + (1.0 - forget[position])[:, :, None] * new_values[position][:, None, :]
        outputs.append(jnp.einsum('hd,hde->he', queries[position], carried, precision=lax.Precision.HIGHEST))
    return (taken, jnp.stack(outputs))

def finish(outputs, head_gain, gate_proj):
    scaled = outputs * lax.rsqrt(lax.optimization_barrier(jnp.mean(outputs * outputs, axis=-1, keepdims=True)) + EPSILON)
    flat = scaled.reshape(gate_proj.shape)
    return (flat * head_gain * jax.nn.silu(gate_proj.astype(jnp.float32))).astype(jnp.bfloat16)

def reference(tokens, norm_gain, w_query, w_forget, w_value, w_gate, lower_bound, head_gain, w_out, state, prev_forget, prev_value, accepted):
    floated = tokens.astype(jnp.float32)
    normed = (floated * lax.rsqrt(lax.optimization_barrier(jnp.mean(floated * floated, axis=-1, keepdims=True)) + EPSILON) * norm_gain).astype(jnp.bfloat16)
    query_proj = jnp.dot(normed, w_query, preferred_element_type=jnp.float32).astype(jnp.bfloat16)
    forget_proj = jnp.dot(normed, w_forget, preferred_element_type=jnp.float32).astype(jnp.bfloat16)
    value_proj = jnp.dot(normed, w_value, preferred_element_type=jnp.float32).astype(jnp.bfloat16)
    gate_proj = jnp.dot(normed, w_gate, preferred_element_type=jnp.float32).astype(jnp.bfloat16)
    seq_total = state.shape[0]
    bounds = lower_bound.reshape(HEADS, KEY_DIM)
    queries = query_proj.astype(jnp.float32).reshape(seq_total, PROPOSALS, HEADS, KEY_DIM) * KEY_DIM ** (-0.5)
    forget = forget_of(forget_proj.reshape(seq_total, PROPOSALS, HEADS, KEY_DIM), bounds)
    new_values = value_proj.astype(jnp.float32).reshape(seq_total, PROPOSALS, HEADS, VAL_DIM)
    old_forget = forget_of(prev_forget.reshape(seq_total, PROPOSALS, HEADS, KEY_DIM), bounds)
    old_values = prev_value.astype(jnp.float32).reshape(seq_total, PROPOSALS, HEADS, VAL_DIM)
    taken, outputs = lax.map(lambda packed: recur_one(*packed), (state, old_forget, old_values, accepted, queries, forget, new_values))
    head_out = finish(outputs, head_gain, gate_proj)
    mixed = jnp.dot(head_out, w_out, preferred_element_type=jnp.float32).astype(jnp.bfloat16)
    return (mixed, taken)
```

```python
import functools

import jax
import jax.numpy as jnp
from jax import lax
from jax.experimental import pallas as pl
from jax.experimental.pallas import tpu as pltpu
from jax.sharding import PartitionSpec as P

EPSILON = 1e-06
MESH = pl.DeviceIdType.MESH
F32 = jnp.float32
BF16 = jnp.bfloat16


def project_kernel(
    nz, ny, ntp,
    x_ref, wq_ref, wf_ref, wv_ref, wg_ref, out_ref,
    wall, xall, to_right, to_left, from_left, from_right,
    own_sem, w_send, w_recv, x_send, x_recv, f_send, f_recv,
    r_send, r_recv, l_send, l_recv,
):
    weights = (wq_ref, wf_ref, wv_ref, wg_ref)
    nw = len(weights)
    kd = wq_ref.shape[0]
    depth = ny * kd
    tokens = x_ref.shape[0]
    rows = tokens // ntp
    kv = lax.axis_index("kv")
    t = lax.axis_index("tp")
    z = kv // ny
    y = kv % ny

    def dev(zz, yy, tt):
        return (zz * ny + yy, tt)

    barrier = pltpu.get_barrier_semaphore()
    for o in range(1, ny):
        pl.semaphore_signal(barrier, inc=1, device_id=dev(z, (y + o) % ny, t), device_id_type=MESH)
    for o in range(1, nz):
        pl.semaphore_signal(barrier, inc=1, device_id=dev((z + o) % nz, y, t), device_id_type=MESH)
    for o in range(1, ntp):
        pl.semaphore_signal(barrier, inc=1, device_id=dev(z, y, (t + o) % ntp), device_id_type=MESH)
    pl.semaphore_wait(barrier, ny + nz + ntp - 3)

    def x_copy(o, at_z, target):
        return pltpu.make_async_remote_copy(
            src_ref=x_ref.at[pl.ds(pl.multiple_of(t * rows, rows), rows), pl.ds(pl.multiple_of(target * depth, depth), depth)],
            dst_ref=xall.at[at_z, pl.ds(pl.multiple_of(t * rows, rows), rows)],
            send_sem=x_send.at[o - 1], recv_sem=x_recv.at[o - 1],
            device_id=dev(target, y, t), device_id_type=MESH,
        )

    def w_copy(o, i, at_y):
        return pltpu.make_async_remote_copy(
            src_ref=weights[i], dst_ref=wall.at[at_y, i],
            send_sem=w_send.at[o - 1, i], recv_sem=w_recv.at[o - 1, i],
            device_id=dev(z, (y + o) % ny, t), device_id_type=MESH,
        )

    def f_copy(o, q, at_t):
        part = xall.at[(z + nz - o) % nz, pl.ds(pl.multiple_of(at_t * rows, rows), rows)]
        return pltpu.make_async_remote_copy(
            src_ref=part, dst_ref=part,
            send_sem=f_send.at[o - 1, q - 1], recv_sem=f_recv.at[o - 1, q - 1],
            device_id=dev(z, y, (t + q) % ntp), device_id_type=MESH,
        )

    for o in range(1, nz):
        x_copy(o, z, (z + o) % nz).start()
    for i in range(nw):
        for o in range(1, ny):
            w_copy(o, i, y).start()
    own_copies = [pltpu.make_async_copy(weights[i], wall.at[y, i], own_sem.at[i]) for i in range(nw)]
    own_copies.append(
        pltpu.make_async_copy(x_ref.at[:, pl.ds(pl.multiple_of(z * depth, depth), depth)], xall.at[z], own_sem.at[nw])
    )
    for copy in own_copies:
        copy.start()
    for o in range(1, nz):
        x_copy(o, (z + nz - o) % nz, (z + o) % nz).wait_recv()
        for q in range(1, ntp):
            f_copy(o, q, t).start()
    for copy in own_copies:
        copy.wait()
    for o in range(1, nz):
        for q in range(1, ntp):
            f_copy(o, q, (t + ntp - q) % ntp).wait_recv()

    def hop(stage, landing, sends, recvs, dest, i, towards):
        return pltpu.make_async_remote_copy(
            src_ref=stage.at[dest, i], dst_ref=landing.at[dest, i],
            send_sem=sends.at[dest, i], recv_sem=recvs.at[dest, i],
            device_id=dev(towards, y, t), device_id_type=MESH,
        )

    def right_hop(dest, i):
        return hop(to_right, from_left, r_send, r_recv, dest, i, jnp.minimum(z + 1, nz - 1))

    def left_hop(dest, i):
        return hop(to_left, from_right, l_send, l_recv, dest, i, jnp.maximum(z - 1, 0))

    def product(dest, i):
        total = None
        for yy in range(ny):
            piece = jnp.dot(
                xall[dest, :, yy * kd:(yy + 1) * kd], wall[yy, i], preferred_element_type=F32
            )
            total = piece if total is None else total + piece
        return total

    def per_weight(i, carry):
        for o in range(1, ny):
            pltpu.make_async_remote_copy(
                src_ref=wq_ref, dst_ref=wall.at[(y + ny - o) % ny, i],
                send_sem=w_send.at[o - 1, i], recv_sem=w_recv.at[o - 1, i],
                device_id=dev(z, (y + o) % ny, t), device_id_type=MESH,
            ).wait_recv()
        for j in range(nz - 1):
            for dest, active, edge, hop_of, landing, stage in (
                (nz - 1 - j, z < nz - 1 - j, z == 0, right_hop, from_left, to_right),
                (j, z > j, z == nz - 1, left_hop, from_right, to_left),
            ):
                @pl.when(active)
                def _():
                    fresh = product(dest, i)

                    @pl.when(edge)
                    def _():
                        stage[dest, i] = fresh.astype(BF16)

                    @pl.when(jnp.logical_not(edge))
                    def _():
                        hop_of(dest, i).wait_recv()
                        stage[dest, i] = (fresh + landing[dest, i].astype(F32)).astype(BF16)

                    hop_of(dest, i).start()
        out_ref[i] = product(z, i).astype(out_ref.dtype)
        return carry

    lax.fori_loop(0, nw, per_weight, 0)

    def finish(i, carry):
        @pl.when(z > 0)
        def _():
            right_hop(z, i).wait_recv()
            out_ref[i] = out_ref[i] + from_left[z, i].astype(F32)

        @pl.when(z < nz - 1)
        def _():
            left_hop(z, i).wait_recv()
            out_ref[i] = out_ref[i] + from_right[z, i].astype(F32)

        return carry

    lax.fori_loop(0, nw, finish, 0)

    for o in range(1, nz):
        x_copy(o, z, (z + o) % nz).wait_send()
        for q in range(1, ntp):
            f_copy(o, q, t).wait_send()
    for i in range(nw):
        for o in range(1, ny):
            w_copy(o, i, y).wait_send()

    def drain(i, carry):
        for dest in range(nz):
            @pl.when(z < dest)
            def _():
                right_hop(dest, i).wait_send()

            @pl.when(z > dest)
            def _():
                left_hop(dest, i).wait_send()
        return carry

    lax.fori_loop(0, nw, drain, 0)


def project(normed, weights, nz, ny, ntp):
    tokens = normed.shape[0]
    kd, cols = weights[0].shape
    nw = len(weights)
    dma = pltpu.SemaphoreType.DMA
    strip = pltpu.VMEM((nz, nw, tokens, cols), BF16)
    return pl.pallas_call(
        functools.partial(project_kernel, nz, ny, ntp),
        out_shape=jax.ShapeDtypeStruct((nw, tokens, cols), F32),
        in_specs=[pl.BlockSpec(memory_space=pltpu.VMEM)] * (1 + nw),
        out_specs=pl.BlockSpec(memory_space=pltpu.VMEM),
        scratch_shapes=[
            pltpu.VMEM((ny, nw, kd, cols), BF16),
            pltpu.VMEM((nz, tokens, ny * kd), BF16),
            strip, strip, strip, strip,
            dma((nw + 1,)),
            dma((ny - 1, nw)), dma((ny - 1, nw)),
            dma((nz - 1,)), dma((nz - 1,)),
            dma((nz - 1, ntp - 1)), dma((nz - 1, ntp - 1)),
            dma((nz, nw)), dma((nz, nw)), dma((nz, nw)), dma((nz, nw)),
        ],
        compiler_params=pltpu.CompilerParams(
            collective_id=0, has_side_effects=True, vmem_limit_bytes=40 * 1024 * 1024
        ),
        cost_estimate=pl.CostEstimate(
            flops=2 * tokens * kd * nz * ny * cols * nw, bytes_accessed=300_000_000, transcendentals=0
        ),
    )(normed, *weights)


def gate_of(pre, bounds):
    return bounds + (1.0 - bounds) * jax.nn.sigmoid(pre.astype(F32))


def split(value):
    high = value.astype(BF16)
    return high, (value - high.astype(F32)).astype(BF16)


def recur_kernel(
    scale, proj_ref, state_ref, pf_ref, pv_ref, acc_ref, bounds_ref, gain_ref,
    head_ref, taken_ref, keys, vals, asks, outs,
):
    steps = pf_ref.shape[0]
    block = state_ref.shape[0]
    bounds = bounds_ref[...]
    accepted = acc_ref[...]

    decay = jnp.ones((block, bounds.shape[-1]), F32)
    for p in reversed(range(steps)):
        gate = gate_of(pf_ref[p], bounds)
        kept = p < accepted
        high, low = split(jnp.where(kept, (1.0 - gate) * decay, 0.0))
        keys[:, p, :] = high.astype(F32)
        keys[:, steps + p, :] = low.astype(F32)
        past = pv_ref[p].astype(F32)
        vals[:, p, :] = past
        vals[:, steps + p, :] = past
        decay = jnp.where(kept, gate * decay, decay)
    decay_t = decay.T

    query, pre, value, gate_in = (
        [proj_ref[i, p].astype(BF16).astype(F32) for p in range(steps)] for i in range(4)
    )
    forget = [gate_of(pre[p], bounds) for p in range(steps)]
    inner = []
    reach = None
    for p in range(steps):
        ask = query[p] * scale
        total = None
        for s in reversed(range(p + 1)):
            weight = jnp.sum(ask * (1.0 - forget[s]), axis=-1, keepdims=True) * value[s]
            total = weight if total is None else total + weight
            ask = ask * forget[s]
        inner.append(total)
        high, low = split(ask)
        asks[:, p, :] = high.astype(F32)
        asks[:, steps + p, :] = low.astype(F32)

    for s in range(block):
        added = lax.dot_general(
            keys[s].astype(BF16), vals[s].astype(BF16), (((0,), (0,)), ((), ())),
            preferred_element_type=F32,
        )
        taken = decay_t[:, s:s + 1] * state_ref[s, 0] + added
        taken_ref[s, 0] = taken
        outs[s] = jnp.dot(asks[s].astype(BF16), taken.astype(BF16), preferred_element_type=F32)

    for p in range(steps):
        result = outs[:, p, :] + outs[:, steps + p, :] + inner[p]
        scaled = result * lax.rsqrt(jnp.mean(result * result, axis=-1, keepdims=True) + EPSILON)
        gated = gate_in[p]
        head_ref[p] = (scaled * gain_ref[...] * (gated * jax.nn.sigmoid(gated))).astype(BF16)


def recur(proj, state, pf, pv, accepted, bounds, gain):
    seqs, heads, kdim, vdim = state.shape
    steps = pf.shape[0]
    block = min(16, seqs)
    small = lambda: pl.BlockSpec((steps, block, kdim), lambda b, h: (0, b, h))
    row = lambda: pl.BlockSpec((1, kdim), lambda b, h: (0, h))
    body = pltpu.VMEM((block, 2 * steps, kdim), F32)
    return pl.pallas_call(
        functools.partial(recur_kernel, kdim ** (-0.5)),
        grid=(seqs // block, heads),
        out_shape=(
            jax.ShapeDtypeStruct((steps, seqs, heads * vdim), BF16),
            jax.ShapeDtypeStruct(state.shape, F32),
        ),
        in_specs=[
            pl.BlockSpec((4, steps, block, kdim), lambda b, h: (0, 0, b, h)),
            pl.BlockSpec((block, 1, kdim, vdim), lambda b, h: (b, h, 0, 0)),
            small(), small(),
            pl.BlockSpec((block, 1), lambda b, h: (b, 0)),
            row(), row(),
        ],
        out_specs=(
            small(),
            pl.BlockSpec((block, 1, kdim, vdim), lambda b, h: (b, h, 0, 0)),
        ),
        scratch_shapes=[body, body, body, body],
        compiler_params=pltpu.CompilerParams(
            dimension_semantics=("arbitrary", "arbitrary"), vmem_limit_bytes=32 * 1024 * 1024
        ),
        cost_estimate=pl.CostEstimate(
            flops=4 * state.size, bytes_accessed=8 * state.size, transcendentals=0
        ),
    )(proj, state, pf, pv, accepted, bounds, gain)


def on_device(
    nz, ny, ntp,
    tokens, norm_gain, w_query, w_forget, w_value, w_gate, lower_bound, head_gain,
    w_out, state, prev_forget, prev_value, accepted,
):
    seqs = state.shape[0]
    steps = prev_forget.shape[1]
    count, width = tokens.shape
    w_out_all = lax.all_gather(w_out, "kv", axis=0, tiled=True)
    floated = tokens.astype(F32)
    normed = (
        floated
        * lax.rsqrt(jnp.mean(floated * floated, axis=-1, keepdims=True) + EPSILON)
        * norm_gain
    ).astype(BF16)
    normed = normed.reshape(seqs, steps, width).transpose(1, 0, 2).reshape(count, width)
    proj = project(normed, (w_query, w_forget, w_value, w_gate), nz, ny, ntp)
    cols = proj.shape[-1]
    head_out, taken = recur(
        proj.reshape(4, steps, seqs, cols),
        state,
        prev_forget.transpose(1, 0, 2),
        prev_value.transpose(1, 0, 2),
        accepted.reshape(seqs, 1),
        lower_bound.reshape(1, cols),
        head_gain.reshape(1, cols),
    )
    gathered = lax.all_gather(head_out.reshape(count, cols), "tp", axis=1, tiled=True)
    mixed = jnp.dot(gathered, w_out_all, preferred_element_type=F32).astype(BF16)
    mixed = mixed.reshape(steps, seqs, -1).transpose(1, 0, 2).reshape(count, -1)
    return mixed, taken


def solution(mesh):
    nkv, ntp = mesh.shape["kv"], mesh.shape["tp"]
    ny = max(d for d in range(1, nkv + 1) if nkv % d == 0 and d * d <= nkv)
    return jax.shard_map(
        functools.partial(on_device, nkv // ny, ny, ntp),
        mesh=mesh,
        in_specs=(
            P("kv", None),
            P(),
            P("kv", "tp"),
            P("kv", "tp"),
            P("kv", "tp"),
            P("kv", "tp"),
            P("tp"),
            P("tp"),
            P("kv", "tp"),
            P("kv", "tp", None, None),
            P("kv", None, "tp"),
            P("kv", None, "tp"),
            P("kv"),
        ),
        out_specs=(P("kv", "tp"), P("kv", "tp", None, None)),
        check_vma=False,
    )
```

```python
import functools

import jax
import jax.numpy as jnp
from jax import lax
from jax.experimental import pallas as pl
from jax.experimental.pallas import tpu as pltpu
from jax.sharding import PartitionSpec as P

EPSILON = 1e-06
MESH = pl.DeviceIdType.MESH
F32 = jnp.float32
BF16 = jnp.bfloat16


def project_kernel(
    nz, ny, ntp,
    x_ref, wq_ref, wf_ref, wv_ref, wg_ref, wo_ref, out_ref, wo_all,
    wall, xall, to_right, to_left, from_left, from_right,
    own_sem, w_send, w_recv, x_send, x_recv, f_send, f_recv,
    r_send, r_recv, l_send, l_recv,
    or_send, or_recv, ol_send, ol_recv, oy_send, oy_recv,
):
    weights = (wq_ref, wf_ref, wv_ref, wg_ref)
    nw = len(weights)
    kd = wq_ref.shape[0]
    depth = ny * kd
    tokens = x_ref.shape[0]
    rows = tokens // ntp
    kv = lax.axis_index("kv")
    t = lax.axis_index("tp")
    z = kv // ny
    y = kv % ny

    def dev(zz, yy, tt):
        return (zz * ny + yy, tt)

    barrier = pltpu.get_barrier_semaphore()
    for o in range(1, ny):
        pl.semaphore_signal(barrier, inc=1, device_id=dev(z, (y + o) % ny, t), device_id_type=MESH)
    for o in range(1, nz):
        pl.semaphore_signal(barrier, inc=1, device_id=dev((z + o) % nz, y, t), device_id_type=MESH)
    for o in range(1, ntp):
        pl.semaphore_signal(barrier, inc=1, device_id=dev(z, y, (t + o) % ntp), device_id_type=MESH)
    pl.semaphore_wait(barrier, ny + nz + ntp - 3)

    def x_copy(o, at_z, target):
        return pltpu.make_async_remote_copy(
            src_ref=x_ref.at[pl.ds(pl.multiple_of(t * rows, rows), rows), pl.ds(pl.multiple_of(target * depth, depth), depth)],
            dst_ref=xall.at[at_z, pl.ds(pl.multiple_of(t * rows, rows), rows)],
            send_sem=x_send.at[o - 1], recv_sem=x_recv.at[o - 1],
            device_id=dev(target, y, t), device_id_type=MESH,
        )

    def w_copy(o, i, at_y):
        return pltpu.make_async_remote_copy(
            src_ref=weights[i], dst_ref=wall.at[at_y, i],
            send_sem=w_send.at[o - 1, i], recv_sem=w_recv.at[o - 1, i],
            device_id=dev(z, (y + o) % ny, t), device_id_type=MESH,
        )

    def f_copy(o, q, at_t):
        part = xall.at[(z + nz - o) % nz, pl.ds(pl.multiple_of(at_t * rows, rows), rows)]
        return pltpu.make_async_remote_copy(
            src_ref=part, dst_ref=part,
            send_sem=f_send.at[o - 1, q - 1], recv_sem=f_recv.at[o - 1, q - 1],
            device_id=dev(z, y, (t + q) % ntp), device_id_type=MESH,
        )

    span = wo_ref.shape[0]

    def place(zz, yy):
        return wo_all.at[pl.ds(pl.multiple_of((zz * ny + yy) * span, span), span)]

    def o_line(zz, towards, sends, recvs, own):
        return pltpu.make_async_remote_copy(
            src_ref=wo_ref if own else place(zz, y), dst_ref=place(zz, y),
            send_sem=sends.at[zz], recv_sem=recvs.at[zz],
            device_id=dev(towards, y, t), device_id_type=MESH,
        )

    def o_right(zz, own=False):
        return o_line(zz, jnp.minimum(z + 1, nz - 1), or_send, or_recv, own)

    def o_left(zz, own=False):
        return o_line(zz, jnp.maximum(z - 1, 0), ol_send, ol_recv, own)

    def o_side(zz, o, at_y, own=False):
        return pltpu.make_async_remote_copy(
            src_ref=wo_ref if own else place(zz, at_y), dst_ref=place(zz, at_y),
            send_sem=oy_send.at[zz, o - 1], recv_sem=oy_recv.at[zz, o - 1],
            device_id=dev(z, (y + o) % ny, t), device_id_type=MESH,
        )

    def o_step(s):
        @pl.when(s == 0)
        def _():
            for o in range(1, ny):
                o_side(z, o, y, True).start()

            @pl.when(z < nz - 1)
            def _():
                o_right(z, True).start()

            @pl.when(z > 0)
            def _():
                o_left(z, True).start()

        @pl.when(jnp.logical_and(s > 0, z - s >= 0))
        def _():
            o_right(z - s).wait_recv()
            for o in range(1, ny):
                o_side(z - s, o, y).start()

            @pl.when(z < nz - 1)
            def _():
                o_right(z - s).start()

        @pl.when(jnp.logical_and(s > 0, z + s < nz))
        def _():
            o_left(z + s).wait_recv()
            for o in range(1, ny):
                o_side(z + s, o, y).start()

            @pl.when(z > 0)
            def _():
                o_left(z + s).start()

    for o in range(1, nz):
        x_copy(o, z, (z + o) % nz).start()
    for i in range(nw):
        for o in range(1, ny):
            w_copy(o, i, y).start()
    own_copies = [pltpu.make_async_copy(weights[i], wall.at[y, i], own_sem.at[i]) for i in range(nw)]
    own_copies.append(
        pltpu.make_async_copy(x_ref.at[:, pl.ds(pl.multiple_of(z * depth, depth), depth)], xall.at[z], own_sem.at[nw])
    )
    own_copies.append(pltpu.make_async_copy(wo_ref, place(z, y), own_sem.at[nw + 1]))
    for copy in own_copies:
        copy.start()
    for o in range(1, nz):
        x_copy(o, (z + nz - o) % nz, (z + o) % nz).wait_recv()
        for q in range(1, ntp):
            f_copy(o, q, t).start()
    for copy in own_copies:
        copy.wait()
    for o in range(1, nz):
        for q in range(1, ntp):
            f_copy(o, q, (t + ntp - q) % ntp).wait_recv()

    def hop(stage, landing, sends, recvs, dest, i, towards):
        return pltpu.make_async_remote_copy(
            src_ref=stage.at[dest, i], dst_ref=landing.at[dest, i],
            send_sem=sends.at[dest, i], recv_sem=recvs.at[dest, i],
            device_id=dev(towards, y, t), device_id_type=MESH,
        )

    def right_hop(dest, i):
        return hop(to_right, from_left, r_send, r_recv, dest, i, jnp.minimum(z + 1, nz - 1))

    def left_hop(dest, i):
        return hop(to_left, from_right, l_send, l_recv, dest, i, jnp.maximum(z - 1, 0))

    def product(dest, i):
        total = None
        for yy in range(ny):
            piece = jnp.dot(
                xall[dest, :, yy * kd:(yy + 1) * kd], wall[yy, i], preferred_element_type=F32
            )
            total = piece if total is None else total + piece
        return total

    def per_weight(i, carry):
        for o in range(1, ny):
            pltpu.make_async_remote_copy(
                src_ref=wq_ref, dst_ref=wall.at[(y + ny - o) % ny, i],
                send_sem=w_send.at[o - 1, i], recv_sem=w_recv.at[o - 1, i],
                device_id=dev(z, (y + o) % ny, t), device_id_type=MESH,
            ).wait_recv()
        for j in range(nz - 1):
            for dest, active, edge, hop_of, landing, stage in (
                (nz - 1 - j, z < nz - 1 - j, z == 0, right_hop, from_left, to_right),
                (j, z > j, z == nz - 1, left_hop, from_right, to_left),
            ):
                @pl.when(active)
                def _():
                    fresh = product(dest, i)

                    @pl.when(edge)
                    def _():
                        stage[dest, i] = fresh.astype(BF16)

                    @pl.when(jnp.logical_not(edge))
                    def _():
                        hop_of(dest, i).wait_recv()
                        stage[dest, i] = (fresh + landing[dest, i].astype(F32)).astype(BF16)

                    hop_of(dest, i).start()
        out_ref[i] = product(z, i).astype(out_ref.dtype)
        o_step(i)
        return carry

    lax.fori_loop(0, nw, per_weight, 0)
    for s in range(nw, nz):
        o_step(s)

    def finish(i, carry):
        @pl.when(z > 0)
        def _():
            right_hop(z, i).wait_recv()
            out_ref[i] = out_ref[i] + from_left[z, i].astype(F32)

        @pl.when(z < nz - 1)
        def _():
            left_hop(z, i).wait_recv()
            out_ref[i] = out_ref[i] + from_right[z, i].astype(F32)

        return carry

    lax.fori_loop(0, nw, finish, 0)

    for o in range(1, nz):
        x_copy(o, z, (z + o) % nz).wait_send()
        for q in range(1, ntp):
            f_copy(o, q, t).wait_send()
    for i in range(nw):
        for o in range(1, ny):
            w_copy(o, i, y).wait_send()

    def drain(i, carry):
        for dest in range(nz):
            @pl.when(z < dest)
            def _():
                right_hop(dest, i).wait_send()

            @pl.when(z > dest)
            def _():
                left_hop(dest, i).wait_send()
        return carry

    lax.fori_loop(0, nw, drain, 0)

    for zz in range(nz):
        for o in range(1, ny):
            o_side(zz, o, (y + ny - o) % ny).wait_recv()
            o_side(zz, o, y).wait_send()

        @pl.when(jnp.logical_and(zz <= z, z < nz - 1))
        def _():
            o_right(zz).wait_send()

        @pl.when(jnp.logical_and(zz >= z, z > 0))
        def _():
            o_left(zz).wait_send()


def project(normed, weights, w_out, nz, ny, ntp):
    tokens = normed.shape[0]
    kd, cols = weights[0].shape
    nw = len(weights)
    dma = pltpu.SemaphoreType.DMA
    strip = pltpu.VMEM((nz, nw, tokens, cols), BF16)
    return pl.pallas_call(
        functools.partial(project_kernel, nz, ny, ntp),
        out_shape=(
            jax.ShapeDtypeStruct((nw, tokens, cols), F32),
            jax.ShapeDtypeStruct((nz * ny * w_out.shape[0], w_out.shape[1]), BF16),
        ),
        in_specs=[pl.BlockSpec(memory_space=pltpu.VMEM)] * (2 + nw),
        out_specs=(pl.BlockSpec(memory_space=pltpu.VMEM),) * 2,
        scratch_shapes=[
            pltpu.VMEM((ny, nw, kd, cols), BF16),
            pltpu.VMEM((nz, tokens, ny * kd), BF16),
            strip, strip, strip, strip,
            dma((nw + 2,)),
            dma((ny - 1, nw)), dma((ny - 1, nw)),
            dma((nz - 1,)), dma((nz - 1,)),
            dma((nz - 1, ntp - 1)), dma((nz - 1, ntp - 1)),
            dma((nz, nw)), dma((nz, nw)), dma((nz, nw)), dma((nz, nw)),
            dma((nz,)), dma((nz,)), dma((nz,)), dma((nz,)),
            dma((nz, ny - 1)), dma((nz, ny - 1)),
        ],
        compiler_params=pltpu.CompilerParams(
            collective_id=0, has_side_effects=True, vmem_limit_bytes=40 * 1024 * 1024
        ),
        cost_estimate=pl.CostEstimate(
            flops=2 * tokens * kd * nz * ny * cols * nw, bytes_accessed=300_000_000, transcendentals=0
        ),
    )(normed, *weights, w_out)


def gate_of(pre, bounds):
    return bounds + (1.0 - bounds) * jax.nn.sigmoid(pre.astype(F32))


def split(value):
    high = value.astype(BF16)
    return high, (value - high.astype(F32)).astype(BF16)


def recur_kernel(
    scale, proj_ref, state_ref, pf_ref, pv_ref, acc_ref, bounds_ref, gain_ref,
    head_ref, taken_ref, keys, vals, asks, outs, flat,
):
    steps = pf_ref.shape[0]
    block = state_ref.shape[0]
    bounds = bounds_ref[...]
    accepted = acc_ref[...]

    decay = jnp.ones((block, bounds.shape[-1]), F32)
    for p in reversed(range(steps)):
        gate = gate_of(pf_ref[p], bounds)
        kept = p < accepted
        high, low = split(jnp.where(kept, (1.0 - gate) * decay, 0.0))
        keys[:, p, :] = high.astype(F32)
        keys[:, steps + p, :] = low.astype(F32)
        past = pv_ref[p].astype(F32)
        vals[:, p, :] = past
        vals[:, steps + p, :] = past
        decay = jnp.where(kept, gate * decay, decay)
    decay_t = decay.T

    query, pre, value, gate_in = (
        [proj_ref[i, pl.ds(p, block, stride=steps), :].astype(BF16).astype(F32) for p in range(steps)] for i in range(4)
    )
    forget = [gate_of(pre[p], bounds) for p in range(steps)]
    inner = []
    reach = None
    for p in range(steps):
        ask = query[p] * scale
        total = None
        for s in reversed(range(p + 1)):
            weight = jnp.sum(ask * (1.0 - forget[s]), axis=-1, keepdims=True) * value[s]
            total = weight if total is None else total + weight
            ask = ask * forget[s]
        inner.append(total)
        high, low = split(ask)
        asks[:, p, :] = high.astype(F32)
        asks[:, steps + p, :] = low.astype(F32)

    for s in range(block):
        added = lax.dot_general(
            keys[s].astype(BF16), vals[s].astype(BF16), (((0,), (0,)), ((), ())),
            preferred_element_type=F32,
        )
        taken = decay_t[:, s:s + 1] * state_ref[s, 0] + added
        taken_ref[s, 0] = taken
        outs[s] = jnp.dot(asks[s].astype(BF16), taken.astype(BF16), preferred_element_type=F32)

    for p in range(steps):
        result = outs[:, p, :] + outs[:, steps + p, :] + inner[p]
        scaled = result * lax.rsqrt(jnp.mean(result * result, axis=-1, keepdims=True) + EPSILON)
        gated = gate_in[p]
        flat[pl.ds(p, block, stride=steps), :] = scaled * gain_ref[...] * (gated * jax.nn.sigmoid(gated))
    head_ref[...] = flat[...].astype(BF16)


def recur(proj, state, pf, pv, accepted, bounds, gain):
    seqs, heads, kdim, vdim = state.shape
    steps = pf.shape[0]
    block = min(16, seqs)
    small = lambda: pl.BlockSpec((steps, block, kdim), lambda b, h: (0, b, h))
    row = lambda: pl.BlockSpec((1, kdim), lambda b, h: (0, h))
    body = pltpu.VMEM((block, 2 * steps, kdim), F32)
    return pl.pallas_call(
        functools.partial(recur_kernel, kdim ** (-0.5)),
        grid=(seqs // block, heads),
        out_shape=(
            jax.ShapeDtypeStruct((steps * seqs, heads * vdim), BF16),
            jax.ShapeDtypeStruct(state.shape, F32),
        ),
        in_specs=[
            pl.BlockSpec((4, steps * block, kdim), lambda b, h: (0, b, h)),
            pl.BlockSpec((block, 1, kdim, vdim), lambda b, h: (b, h, 0, 0)),
            small(), small(),
            pl.BlockSpec((block, 1), lambda b, h: (b, 0)),
            row(), row(),
        ],
        out_specs=(
            pl.BlockSpec((steps * block, vdim), lambda b, h: (b, h)),
            pl.BlockSpec((block, 1, kdim, vdim), lambda b, h: (b, h, 0, 0)),
        ),
        scratch_shapes=[body, body, body, body, pltpu.VMEM((steps * block, vdim), F32)],
        compiler_params=pltpu.CompilerParams(
            dimension_semantics=("arbitrary", "arbitrary"), vmem_limit_bytes=42 * 1024 * 1024
        ),
        cost_estimate=pl.CostEstimate(
            flops=4 * state.size, bytes_accessed=8 * state.size, transcendentals=0
        ),
    )(proj, state, pf, pv, accepted, bounds, gain)


def combine_kernel(ntp, head_ref, w_ref, mixed_ref, landed, total, sends, recvs):
    kv = lax.axis_index("kv")
    t = lax.axis_index("tp")
    cols = head_ref.shape[1]
    barrier = pltpu.get_barrier_semaphore()
    for q in range(1, ntp):
        pl.semaphore_signal(barrier, inc=1, device_id=(kv, (t + q) % ntp), device_id_type=MESH)
    pl.semaphore_wait(barrier, ntp - 1)

    def copy(q):
        return pltpu.make_async_remote_copy(
            src_ref=head_ref, dst_ref=landed.at[q - 1],
            send_sem=sends.at[q - 1], recv_sem=recvs.at[q - 1],
            device_id=(kv, (t + q) % ntp), device_id_type=MESH,
        )

    def part(source):
        return w_ref[pl.ds(pl.multiple_of(source * cols, cols), cols), :]

    for q in range(1, ntp):
        copy(q).start()
    total[...] = jnp.dot(head_ref[...], part(t), preferred_element_type=F32)
    for q in range(1, ntp):
        copy(q).wait_recv()
        total[...] += jnp.dot(landed[q - 1], part((t + ntp - q) % ntp), preferred_element_type=F32)
    mixed_ref[...] = total[...].astype(BF16)
    for q in range(1, ntp):
        copy(q).wait_send()


def combine(head, w_all, ntp):
    count, cols = head.shape
    width = w_all.shape[1]
    dma = pltpu.SemaphoreType.DMA
    return pl.pallas_call(
        functools.partial(combine_kernel, ntp),
        out_shape=jax.ShapeDtypeStruct((count, width), BF16),
        in_specs=[pl.BlockSpec(memory_space=pltpu.VMEM)] * 2,
        out_specs=pl.BlockSpec(memory_space=pltpu.VMEM),
        scratch_shapes=[
            pltpu.VMEM((ntp - 1, count, cols), BF16),
            pltpu.VMEM((count, width), F32),
            dma((ntp - 1,)), dma((ntp - 1,)),
        ],
        compiler_params=pltpu.CompilerParams(
            collective_id=1, has_side_effects=True, vmem_limit_bytes=24 * 1024 * 1024
        ),
        cost_estimate=pl.CostEstimate(
            flops=2 * w_all.size * count, bytes_accessed=40_000_000, transcendentals=0
        ),
    )(head, w_all)


def on_device(
    nz, ny, ntp,
    tokens, norm_gain, w_query, w_forget, w_value, w_gate, lower_bound, head_gain,
    w_out, state, prev_forget, prev_value, accepted,
):
    seqs = state.shape[0]
    floated = tokens.astype(F32)
    normed = (
        floated
        * lax.rsqrt(jnp.mean(floated * floated, axis=-1, keepdims=True) + EPSILON)
        * norm_gain
    ).astype(BF16)
    proj, w_all = project(normed, (w_query, w_forget, w_value, w_gate), w_out, nz, ny, ntp)
    cols = proj.shape[-1]
    head_out, taken = recur(
        proj,
        state,
        prev_forget.transpose(1, 0, 2),
        prev_value.transpose(1, 0, 2),
        accepted.reshape(seqs, 1),
        lower_bound.reshape(1, cols),
        head_gain.reshape(1, cols),
    )
    mixed = combine(head_out, w_all, ntp)
    return mixed, taken


def solution(mesh):
    nkv, ntp = mesh.shape["kv"], mesh.shape["tp"]
    ny = max(d for d in range(1, nkv + 1) if nkv % d == 0 and d * d <= nkv)
    return jax.shard_map(
        functools.partial(on_device, nkv // ny, ny, ntp),
        mesh=mesh,
        in_specs=(
            P("kv", None),
            P(),
            P("kv", "tp"),
            P("kv", "tp"),
            P("kv", "tp"),
            P("kv", "tp"),
            P("tp"),
            P("tp"),
            P("kv", "tp"),
            P("kv", "tp", None, None),
            P("kv", None, "tp"),
            P("kv", None, "tp"),
            P("kv"),
        ),
        out_specs=(P("kv", "tp"), P("kv", "tp", None, None)),
        check_vma=False,
    )
```

```python
import functools

import jax
import jax.numpy as jnp
from jax import lax
from jax.experimental import pallas as pl
from jax.experimental.pallas import tpu as pltpu
from jax.sharding import PartitionSpec as P

EPSILON = 1e-06
MESH = pl.DeviceIdType.MESH
F32 = jnp.float32
BF16 = jnp.bfloat16


def project_kernel(
    nz, ny, ntp,
    x_ref, wq_ref, wf_ref, wv_ref, wg_ref, wo_ref, out_ref, wo_all,
    wall, xall, to_right, to_left, from_left, from_right,
    own_sem, w_send, w_recv, x_send, x_recv, f_send, f_recv,
    r_send, r_recv, l_send, l_recv,
    or_send, or_recv, ol_send, ol_recv, oy_send, oy_recv,
):
    weights = (wq_ref, wf_ref, wv_ref, wg_ref)
    nw = len(weights)
    kd = wq_ref.shape[0]
    depth = ny * kd
    tokens = x_ref.shape[0]
    rows = tokens // ntp
    kv = lax.axis_index("kv")
    t = lax.axis_index("tp")
    z = kv // ny
    y = kv % ny

    def dev(zz, yy, tt):
        return (zz * ny + yy, tt)

    barrier = pltpu.get_barrier_semaphore()
    for o in range(1, ny):
        pl.semaphore_signal(barrier, inc=1, device_id=dev(z, (y + o) % ny, t), device_id_type=MESH)
    for o in range(1, nz):
        pl.semaphore_signal(barrier, inc=1, device_id=dev((z + o) % nz, y, t), device_id_type=MESH)
    for o in range(1, ntp):
        pl.semaphore_signal(barrier, inc=1, device_id=dev(z, y, (t + o) % ntp), device_id_type=MESH)
    pl.semaphore_wait(barrier, ny + nz + ntp - 3)

    def x_copy(o, at_z, target):
        return pltpu.make_async_remote_copy(
            src_ref=x_ref.at[pl.ds(pl.multiple_of(t * rows, rows), rows), pl.ds(pl.multiple_of(target * depth, depth), depth)],
            dst_ref=xall.at[at_z, pl.ds(pl.multiple_of(t * rows, rows), rows)],
            send_sem=x_send.at[o - 1], recv_sem=x_recv.at[o - 1],
            device_id=dev(target, y, t), device_id_type=MESH,
        )

    def w_copy(o, i, at_y):
        return pltpu.make_async_remote_copy(
            src_ref=weights[i], dst_ref=wall.at[at_y, i],
            send_sem=w_send.at[o - 1, i], recv_sem=w_recv.at[o - 1, i],
            device_id=dev(z, (y + o) % ny, t), device_id_type=MESH,
        )

    def f_copy(o, q, at_t):
        part = xall.at[(z + nz - o) % nz, pl.ds(pl.multiple_of(at_t * rows, rows), rows)]
        return pltpu.make_async_remote_copy(
            src_ref=part, dst_ref=part,
            send_sem=f_send.at[o - 1, q - 1], recv_sem=f_recv.at[o - 1, q - 1],
            device_id=dev(z, y, (t + q) % ntp), device_id_type=MESH,
        )

    span = wo_ref.shape[0]

    def place(zz, yy):
        return wo_all.at[pl.ds(pl.multiple_of((zz * ny + yy) * span, span), span)]

    def o_line(zz, towards, sends, recvs, own):
        return pltpu.make_async_remote_copy(
            src_ref=wo_ref if own else place(zz, y), dst_ref=place(zz, y),
            send_sem=sends.at[zz], recv_sem=recvs.at[zz],
            device_id=dev(towards, y, t), device_id_type=MESH,
        )

    def o_right(zz, own=False):
        return o_line(zz, jnp.minimum(z + 1, nz - 1), or_send, or_recv, own)

    def o_left(zz, own=False):
        return o_line(zz, jnp.maximum(z - 1, 0), ol_send, ol_recv, own)

    def o_side(zz, o, at_y, own=False):
        return pltpu.make_async_remote_copy(
            src_ref=wo_ref if own else place(zz, at_y), dst_ref=place(zz, at_y),
            send_sem=oy_send.at[zz, o - 1], recv_sem=oy_recv.at[zz, o - 1],
            device_id=dev(z, (y + o) % ny, t), device_id_type=MESH,
        )

    def o_step(s):
        @pl.when(s == 0)
        def _():
            for o in range(1, ny):
                o_side(z, o, y, True).start()

        @pl.when(jnp.logical_and(s > 0, z - s >= 0))
        def _():
            o_right(z - s).wait_recv()
            for o in range(1, ny):
                o_side(z - s, o, y).start()

            @pl.when(z < nz - 1)
            def _():
                o_right(z - s).start()

        @pl.when(jnp.logical_and(s > 0, z + s < nz))
        def _():
            o_left(z + s).wait_recv()
            for o in range(1, ny):
                o_side(z + s, o, y).start()

            @pl.when(z > 0)
            def _():
                o_left(z + s).start()

    for o in range(1, nz):
        x_copy(o, z, (z + o) % nz).start()
    for o in range(1, ny):
        w_copy(o, 0, y).start()
    own_copies = [pltpu.make_async_copy(weights[i], wall.at[y, i], own_sem.at[i]) for i in range(nw)]
    own_copies.append(
        pltpu.make_async_copy(x_ref.at[:, pl.ds(pl.multiple_of(z * depth, depth), depth)], xall.at[z], own_sem.at[nw])
    )
    own_copies.append(pltpu.make_async_copy(wo_ref, place(z, y), own_sem.at[nw + 1]))
    for copy in own_copies:
        copy.start()
    for o in range(1, nz):
        x_copy(o, (z + nz - o) % nz, (z + o) % nz).wait_recv()
        for q in range(1, ntp):
            f_copy(o, q, t).start()
    for copy in own_copies:
        copy.wait()
    for o in range(1, ny):
        w_copy(o, 1, y).start()

    @pl.when(z < nz - 1)
    def _():
        o_right(z, True).start()

    @pl.when(z > 0)
    def _():
        o_left(z, True).start()

    def hop(stage, landing, sends, recvs, dest, i, towards):
        return pltpu.make_async_remote_copy(
            src_ref=stage.at[dest, i], dst_ref=landing.at[dest, i],
            send_sem=sends.at[dest, i], recv_sem=recvs.at[dest, i],
            device_id=dev(towards, y, t), device_id_type=MESH,
        )

    def right_hop(dest, i):
        return hop(to_right, from_left, r_send, r_recv, dest, i, jnp.minimum(z + 1, nz - 1))

    def left_hop(dest, i):
        return hop(to_left, from_right, l_send, l_recv, dest, i, jnp.maximum(z - 1, 0))

    def product(dest, i):
        total = None
        for yy in range(ny):
            piece = jnp.dot(
                xall[dest, :, yy * kd:(yy + 1) * kd], wall[yy, i], preferred_element_type=F32
            )
            total = piece if total is None else total + piece
        return total

    def per_weight(i, carry):
        for o in range(1, ny):
            pltpu.make_async_remote_copy(
                src_ref=wq_ref, dst_ref=wall.at[(y + ny - o) % ny, i],
                send_sem=w_send.at[o - 1, i], recv_sem=w_recv.at[o - 1, i],
                device_id=dev(z, (y + o) % ny, t), device_id_type=MESH,
            ).wait_recv()
        for k in range(2, nw):
            @pl.when(i == k - 2)
            def _():
                for o in range(1, ny):
                    w_copy(o, k, y).start()
        for j in range(nz - 1):
            for dest, active, edge, hop_of, landing, stage in (
                (nz - 1 - j, z < nz - 1 - j, z == 0, right_hop, from_left, to_right),
                (j, z > j, z == nz - 1, left_hop, from_right, to_left),
            ):
                @pl.when(active)
                def _():
                    @pl.when(i == 0)
                    def _():
                        o = (z + nz - dest) % nz
                        for q in range(1, ntp):
                            f_copy(o, q, (t + ntp - q) % ntp).wait_recv()

                    fresh = product(dest, i)

                    @pl.when(edge)
                    def _():
                        stage[dest, i] = fresh.astype(BF16)

                    @pl.when(jnp.logical_not(edge))
                    def _():
                        hop_of(dest, i).wait_recv()
                        stage[dest, i] = (fresh + landing[dest, i].astype(F32)).astype(BF16)

                    hop_of(dest, i).start()
        out_ref[i] = product(z, i).astype(out_ref.dtype)
        o_step(i)
        return carry

    lax.fori_loop(0, nw, per_weight, 0)
    for s in range(nw, nz):
        o_step(s)

    def finish(i, carry):
        @pl.when(z > 0)
        def _():
            right_hop(z, i).wait_recv()
            out_ref[i] = out_ref[i] + from_left[z, i].astype(F32)

        @pl.when(z < nz - 1)
        def _():
            left_hop(z, i).wait_recv()
            out_ref[i] = out_ref[i] + from_right[z, i].astype(F32)

        return carry

    lax.fori_loop(0, nw, finish, 0)

    for o in range(1, nz):
        x_copy(o, z, (z + o) % nz).wait_send()
        for q in range(1, ntp):
            f_copy(o, q, t).wait_send()
    for i in range(nw):
        for o in range(1, ny):
            w_copy(o, i, y).wait_send()

    def drain(i, carry):
        for dest in range(nz):
            @pl.when(z < dest)
            def _():
                right_hop(dest, i).wait_send()

            @pl.when(z > dest)
            def _():
                left_hop(dest, i).wait_send()
        return carry

    lax.fori_loop(0, nw, drain, 0)

    for zz in range(nz):
        for o in range(1, ny):
            o_side(zz, o, (y + ny - o) % ny).wait_recv()
            o_side(zz, o, y).wait_send()

        @pl.when(jnp.logical_and(zz <= z, z < nz - 1))
        def _():
            o_right(zz).wait_send()

        @pl.when(jnp.logical_and(zz >= z, z > 0))
        def _():
            o_left(zz).wait_send()


def project(normed, weights, w_out, nz, ny, ntp):
    tokens = normed.shape[0]
    kd, cols = weights[0].shape
    nw = len(weights)
    dma = pltpu.SemaphoreType.DMA
    strip = pltpu.VMEM((nz, nw, tokens, cols), BF16)
    return pl.pallas_call(
        functools.partial(project_kernel, nz, ny, ntp),
        out_shape=(
            jax.ShapeDtypeStruct((nw, tokens, cols), F32),
            jax.ShapeDtypeStruct((nz * ny * w_out.shape[0], w_out.shape[1]), BF16),
        ),
        in_specs=[pl.BlockSpec(memory_space=pltpu.VMEM)] * (2 + nw),
        out_specs=(pl.BlockSpec(memory_space=pltpu.VMEM),) * 2,
        scratch_shapes=[
            pltpu.VMEM((ny, nw, kd, cols), BF16),
            pltpu.VMEM((nz, tokens, ny * kd), BF16),
            strip, strip, strip, strip,
            dma((nw + 2,)),
            dma((ny - 1, nw)), dma((ny - 1, nw)),
            dma((nz - 1,)), dma((nz - 1,)),
            dma((nz - 1, ntp - 1)), dma((nz - 1, ntp - 1)),
            dma((nz, nw)), dma((nz, nw)), dma((nz, nw)), dma((nz, nw)),
            dma((nz,)), dma((nz,)), dma((nz,)), dma((nz,)),
            dma((nz, ny - 1)), dma((nz, ny - 1)),
        ],
        compiler_params=pltpu.CompilerParams(
            collective_id=0, has_side_effects=True, vmem_limit_bytes=40 * 1024 * 1024
        ),
        cost_estimate=pl.CostEstimate(
            flops=2 * tokens * kd * nz * ny * cols * nw, bytes_accessed=300_000_000, transcendentals=0
        ),
    )(normed, *weights, w_out)


def gate_of(pre, bounds):
    return bounds + (1.0 - bounds) * jax.nn.sigmoid(pre.astype(F32))


def split(value):
    high = value.astype(BF16)
    return high, (value - high.astype(F32)).astype(BF16)


def recur_kernel(
    scale, proj_ref, state_ref, pf_ref, pv_ref, acc_ref, bounds_ref, gain_ref,
    head_ref, taken_ref, keys, vals, asks, outs, flat,
):
    steps = pf_ref.shape[0]
    block = state_ref.shape[0]
    bounds = bounds_ref[...]
    accepted = acc_ref[...]

    decay = jnp.ones((block, bounds.shape[-1]), F32)
    for p in reversed(range(steps)):
        gate = gate_of(pf_ref[p], bounds)
        kept = p < accepted
        high, low = split(jnp.where(kept, (1.0 - gate) * decay, 0.0))
        keys[:, p, :] = high.astype(F32)
        keys[:, steps + p, :] = low.astype(F32)
        past = pv_ref[p].astype(F32)
        vals[:, p, :] = past
        vals[:, steps + p, :] = past
        decay = jnp.where(kept, gate * decay, decay)
    decay_t = decay.T

    query, pre, value, gate_in = (
        [proj_ref[i, pl.ds(p, block, stride=steps), :].astype(BF16).astype(F32) for p in range(steps)] for i in range(4)
    )
    forget = [gate_of(pre[p], bounds) for p in range(steps)]
    inner = []
    reach = None
    for p in range(steps):
        ask = query[p] * scale
        total = None
        for s in reversed(range(p + 1)):
            weight = jnp.sum(ask * (1.0 - forget[s]), axis=-1, keepdims=True) * value[s]
            total = weight if total is None else total + weight
            ask = ask * forget[s]
        inner.append(total)
        high, low = split(ask)
        asks[:, p, :] = high.astype(F32)
        asks[:, steps + p, :] = low.astype(F32)

    for s in range(block):
        added = lax.dot_general(
            keys[s].astype(BF16), vals[s].astype(BF16), (((0,), (0,)), ((), ())),
            preferred_element_type=F32,
        )
        taken = decay_t[:, s:s + 1] * state_ref[s, 0] + added
        taken_ref[s, 0] = taken
        outs[s] = jnp.dot(asks[s].astype(BF16), taken.astype(BF16), preferred_element_type=F32)

    for p in range(steps):
        result = outs[:, p, :] + outs[:, steps + p, :] + inner[p]
        scaled = result * lax.rsqrt(jnp.mean(result * result, axis=-1, keepdims=True) + EPSILON)
        gated = gate_in[p]
        flat[pl.ds(p, block, stride=steps), :] = scaled * gain_ref[...] * (gated * jax.nn.sigmoid(gated))
    head_ref[...] = flat[...].astype(BF16)


def recur(proj, state, pf, pv, accepted, bounds, gain):
    seqs, heads, kdim, vdim = state.shape
    steps = pf.shape[0]
    block = min(16, seqs)
    small = lambda: pl.BlockSpec((steps, block, kdim), lambda b, h: (0, b, h))
    row = lambda: pl.BlockSpec((1, kdim), lambda b, h: (0, h))
    body = pltpu.VMEM((block, 2 * steps, kdim), F32)
    return pl.pallas_call(
        functools.partial(recur_kernel, kdim ** (-0.5)),
        grid=(seqs // block, heads),
        out_shape=(
            jax.ShapeDtypeStruct((steps * seqs, heads * vdim), BF16),
            jax.ShapeDtypeStruct(state.shape, F32),
        ),
        in_specs=[
            pl.BlockSpec((4, steps * block, kdim), lambda b, h: (0, b, h)),
            pl.BlockSpec((block, 1, kdim, vdim), lambda b, h: (b, h, 0, 0)),
            small(), small(),
            pl.BlockSpec((block, 1), lambda b, h: (b, 0)),
            row(), row(),
        ],
        out_specs=(
            pl.BlockSpec((steps * block, vdim), lambda b, h: (b, h)),
            pl.BlockSpec((block, 1, kdim, vdim), lambda b, h: (b, h, 0, 0)),
        ),
        scratch_shapes=[body, body, body, body, pltpu.VMEM((steps * block, vdim), F32)],
        compiler_params=pltpu.CompilerParams(
            dimension_semantics=("arbitrary", "arbitrary"), vmem_limit_bytes=42 * 1024 * 1024
        ),
        cost_estimate=pl.CostEstimate(
            flops=4 * state.size, bytes_accessed=8 * state.size, transcendentals=0
        ),
    )(proj, state, pf, pv, accepted, bounds, gain)


def combine_kernel(ntp, head_ref, w_ref, mixed_ref, landed, total, sends, recvs):
    kv = lax.axis_index("kv")
    t = lax.axis_index("tp")
    cols = head_ref.shape[1]
    barrier = pltpu.get_barrier_semaphore()
    for q in range(1, ntp):
        pl.semaphore_signal(barrier, inc=1, device_id=(kv, (t + q) % ntp), device_id_type=MESH)
    pl.semaphore_wait(barrier, ntp - 1)

    def copy(q):
        return pltpu.make_async_remote_copy(
            src_ref=head_ref, dst_ref=landed.at[q - 1],
            send_sem=sends.at[q - 1], recv_sem=recvs.at[q - 1],
            device_id=(kv, (t + q) % ntp), device_id_type=MESH,
        )

    def part(source):
        return w_ref[pl.ds(pl.multiple_of(source * cols, cols), cols), :]

    for q in range(1, ntp):
        copy(q).start()
    total[...] = jnp.dot(head_ref[...], part(t), preferred_element_type=F32)
    for q in range(1, ntp):
        copy(q).wait_recv()
        total[...] += jnp.dot(landed[q - 1], part((t + ntp - q) % ntp), preferred_element_type=F32)
    mixed_ref[...] = total[...].astype(BF16)
    for q in range(1, ntp):
        copy(q).wait_send()


def combine(head, w_all, ntp):
    count, cols = head.shape
    width = w_all.shape[1]
    dma = pltpu.SemaphoreType.DMA
    return pl.pallas_call(
        functools.partial(combine_kernel, ntp),
        out_shape=jax.ShapeDtypeStruct((count, width), BF16),
        in_specs=[pl.BlockSpec(memory_space=pltpu.VMEM)] * 2,
        out_specs=pl.BlockSpec(memory_space=pltpu.VMEM),
        scratch_shapes=[
            pltpu.VMEM((ntp - 1, count, cols), BF16),
            pltpu.VMEM((count, width), F32),
            dma((ntp - 1,)), dma((ntp - 1,)),
        ],
        compiler_params=pltpu.CompilerParams(
            collective_id=1, has_side_effects=True, vmem_limit_bytes=24 * 1024 * 1024
        ),
        cost_estimate=pl.CostEstimate(
            flops=2 * w_all.size * count, bytes_accessed=40_000_000, transcendentals=0
        ),
    )(head, w_all)


def on_device(
    nz, ny, ntp,
    tokens, norm_gain, w_query, w_forget, w_value, w_gate, lower_bound, head_gain,
    w_out, state, prev_forget, prev_value, accepted,
):
    seqs = state.shape[0]
    floated = tokens.astype(F32)
    normed = (
        floated
        * lax.rsqrt(jnp.mean(floated * floated, axis=-1, keepdims=True) + EPSILON)
        * norm_gain
    ).astype(BF16)
    proj, w_all = project(normed, (w_query, w_forget, w_value, w_gate), w_out, nz, ny, ntp)
    cols = proj.shape[-1]
    head_out, taken = recur(
        proj,
        state,
        prev_forget.transpose(1, 0, 2),
        prev_value.transpose(1, 0, 2),
        accepted.reshape(seqs, 1),
        lower_bound.reshape(1, cols),
        head_gain.reshape(1, cols),
    )
    mixed = combine(head_out, w_all, ntp)
    return mixed, taken


def solution(mesh):
    nkv, ntp = mesh.shape["kv"], mesh.shape["tp"]
    ny = max(d for d in range(1, nkv + 1) if nkv % d == 0 and d * d <= nkv)
    return jax.shard_map(
        functools.partial(on_device, nkv // ny, ny, ntp),
        mesh=mesh,
        in_specs=(
            P("kv", None),
            P(),
            P("kv", "tp"),
            P("kv", "tp"),
            P("kv", "tp"),
            P("kv", "tp"),
            P("tp"),
            P("tp"),
            P("kv", "tp"),
            P("kv", "tp", None, None),
            P("kv", None, "tp"),
            P("kv", None, "tp"),
            P("kv"),
        ),
        out_specs=(P("kv", "tp"), P("kv", "tp", None, None)),
        check_vma=False,
    )
```

```python
import functools

import jax
import jax.numpy as jnp
from jax import lax
from jax.experimental import pallas as pl
from jax.experimental.pallas import tpu as pltpu
from jax.sharding import PartitionSpec as P

EPSILON = 1e-06
MESH = pl.DeviceIdType.MESH
F32 = jnp.float32
BF16 = jnp.bfloat16


def project_kernel(
    nz, ny, ntp,
    x_ref, wq_ref, wf_ref, wv_ref, wg_ref, wo_ref, out_ref, wo_all,
    wall, xall, to_right, to_left, from_left, from_right,
    own_sem, w_send, w_recv, x_send, x_recv, f_send, f_recv,
    r_send, r_recv, l_send, l_recv,
    or_send, or_recv, ol_send, ol_recv, oy_send, oy_recv,
):
    weights = (wq_ref, wf_ref, wv_ref, wg_ref)
    nw = len(weights)
    kd = wq_ref.shape[0]
    depth = ny * kd
    tokens = x_ref.shape[0]
    rows = tokens // ntp
    kv = lax.axis_index("kv")
    t = lax.axis_index("tp")
    z = kv // ny
    y = kv % ny

    def dev(zz, yy, tt):
        return (zz * ny + yy, tt)

    barrier = pltpu.get_barrier_semaphore()
    for o in range(1, ny):
        pl.semaphore_signal(barrier, inc=1, device_id=dev(z, (y + o) % ny, t), device_id_type=MESH)
    for o in range(1, nz):
        pl.semaphore_signal(barrier, inc=1, device_id=dev((z + o) % nz, y, t), device_id_type=MESH)
    for o in range(1, ntp):
        pl.semaphore_signal(barrier, inc=1, device_id=dev(z, y, (t + o) % ntp), device_id_type=MESH)
    pl.semaphore_wait(barrier, ny + nz + ntp - 3)

    def x_copy(o, at_z, target):
        return pltpu.make_async_remote_copy(
            src_ref=x_ref.at[pl.ds(pl.multiple_of(t * rows, rows), rows), pl.ds(pl.multiple_of(target * depth, depth), depth)],
            dst_ref=xall.at[at_z, pl.ds(pl.multiple_of(t * rows, rows), rows)],
            send_sem=x_send.at[o - 1], recv_sem=x_recv.at[o - 1],
            device_id=dev(target, y, t), device_id_type=MESH,
        )

    def w_copy(o, i, at_y):
        return pltpu.make_async_remote_copy(
            src_ref=weights[i], dst_ref=wall.at[at_y, i],
            send_sem=w_send.at[o - 1, i], recv_sem=w_recv.at[o - 1, i],
            device_id=dev(z, (y + o) % ny, t), device_id_type=MESH,
        )

    def f_copy(o, q, at_t):
        part = xall.at[(z + nz - o) % nz, pl.ds(pl.multiple_of(at_t * rows, rows), rows)]
        return pltpu.make_async_remote_copy(
            src_ref=part, dst_ref=part,
            send_sem=f_send.at[o - 1, q - 1], recv_sem=f_recv.at[o - 1, q - 1],
            device_id=dev(z, y, (t + q) % ntp), device_id_type=MESH,
        )

    span = wo_ref.shape[0]

    def place(zz, yy):
        return wo_all.at[pl.ds(pl.multiple_of((zz * ny + yy) * span, span), span)]

    def o_line(zz, towards, sends, recvs, own):
        return pltpu.make_async_remote_copy(
            src_ref=wo_ref if own else place(zz, y), dst_ref=place(zz, y),
            send_sem=sends.at[zz], recv_sem=recvs.at[zz],
            device_id=dev(towards, y, t), device_id_type=MESH,
        )

    def o_right(zz, own=False):
        return o_line(zz, jnp.minimum(z + 1, nz - 1), or_send, or_recv, own)

    def o_left(zz, own=False):
        return o_line(zz, jnp.maximum(z - 1, 0), ol_send, ol_recv, own)

    def o_side(zz, o, at_y, own=False):
        return pltpu.make_async_remote_copy(
            src_ref=wo_ref if own else place(zz, at_y), dst_ref=place(zz, at_y),
            send_sem=oy_send.at[zz, o - 1], recv_sem=oy_recv.at[zz, o - 1],
            device_id=dev(z, (y + o) % ny, t), device_id_type=MESH,
        )

    def o_step(s):
        @pl.when(s == 0)
        def _():
            for o in range(1, ny):
                o_side(z, o, y, True).start()

        @pl.when(jnp.logical_and(s > 0, z - s >= 0))
        def _():
            o_right(z - s).wait_recv()
            for o in range(1, ny):
                o_side(z - s, o, y).start()

            @pl.when(z < nz - 1)
            def _():
                o_right(z - s).start()

        @pl.when(jnp.logical_and(s > 0, z + s < nz))
        def _():
            o_left(z + s).wait_recv()
            for o in range(1, ny):
                o_side(z + s, o, y).start()

            @pl.when(z > 0)
            def _():
                o_left(z + s).start()

    for o in range(1, nz):
        x_copy(o, z, (z + o) % nz).start()
    for o in range(1, ny):
        w_copy(o, 0, y).start()
    own_copies = [pltpu.make_async_copy(weights[i], wall.at[y, i], own_sem.at[i]) for i in range(nw)]
    own_copies.append(
        pltpu.make_async_copy(x_ref.at[:, pl.ds(pl.multiple_of(z * depth, depth), depth)], xall.at[z], own_sem.at[nw])
    )
    own_copies.append(pltpu.make_async_copy(wo_ref, place(z, y), own_sem.at[nw + 1]))
    for copy in own_copies:
        copy.start()
    for o in range(1, nz):
        x_copy(o, (z + nz - o) % nz, (z + o) % nz).wait_recv()
        for q in range(1, ntp):
            f_copy(o, q, t).start()
    for copy in own_copies:
        copy.wait()
    for o in range(1, ny):
        w_copy(o, 1, y).start()

    @pl.when(z < nz - 1)
    def _():
        o_right(z, True).start()

    @pl.when(z > 0)
    def _():
        o_left(z, True).start()

    def hop(stage, landing, sends, recvs, dest, i, towards):
        return pltpu.make_async_remote_copy(
            src_ref=stage.at[dest, i], dst_ref=landing.at[dest, i],
            send_sem=sends.at[dest, i], recv_sem=recvs.at[dest, i],
            device_id=dev(towards, y, t), device_id_type=MESH,
        )

    def right_hop(dest, i):
        return hop(to_right, from_left, r_send, r_recv, dest, i, jnp.minimum(z + 1, nz - 1))

    def left_hop(dest, i):
        return hop(to_left, from_right, l_send, l_recv, dest, i, jnp.maximum(z - 1, 0))

    def product(dest, i):
        total = None
        for yy in range(ny):
            piece = jnp.dot(
                xall[dest, :, yy * kd:(yy + 1) * kd], wall[yy, i], preferred_element_type=F32
            )
            total = piece if total is None else total + piece
        return total

    def per_weight(i, carry):
        for o in range(1, ny):
            pltpu.make_async_remote_copy(
                src_ref=wq_ref, dst_ref=wall.at[(y + ny - o) % ny, i],
                send_sem=w_send.at[o - 1, i], recv_sem=w_recv.at[o - 1, i],
                device_id=dev(z, (y + o) % ny, t), device_id_type=MESH,
            ).wait_recv()
        for k in range(2, nw):
            @pl.when(i == k - 2)
            def _():
                for o in range(1, ny):
                    w_copy(o, k, y).start()
        for j in range(nz - 1):
            for dest, active, edge, hop_of, landing, stage in (
                (nz - 1 - j, z < nz - 1 - j, z == 0, right_hop, from_left, to_right),
                (j, z > j, z == nz - 1, left_hop, from_right, to_left),
            ):
                @pl.when(active)
                def _():
                    @pl.when(i == 0)
                    def _():
                        o = (z + nz - dest) % nz
                        for q in range(1, ntp):
                            f_copy(o, q, (t + ntp - q) % ntp).wait_recv()

                    fresh = product(dest, i)

                    @pl.when(edge)
                    def _():
                        stage[dest, i] = fresh.astype(BF16)

                    @pl.when(jnp.logical_not(edge))
                    def _():
                        hop_of(dest, i).wait_recv()
                        stage[dest, i] = (fresh + landing[dest, i].astype(F32)).astype(BF16)

                    hop_of(dest, i).start()
        out_ref[i] = product(z, i).astype(out_ref.dtype)
        o_step(i)
        return carry

    lax.fori_loop(0, nw, per_weight, 0)
    for s in range(nw, nz):
        o_step(s)

    def finish(i, carry):
        @pl.when(z > 0)
        def _():
            right_hop(z, i).wait_recv()
            out_ref[i] = out_ref[i] + from_left[z, i].astype(F32)

        @pl.when(z < nz - 1)
        def _():
            left_hop(z, i).wait_recv()
            out_ref[i] = out_ref[i] + from_right[z, i].astype(F32)

        return carry

    lax.fori_loop(0, nw, finish, 0)

    for o in range(1, nz):
        x_copy(o, z, (z + o) % nz).wait_send()
        for q in range(1, ntp):
            f_copy(o, q, t).wait_send()
    for i in range(nw):
        for o in range(1, ny):
            w_copy(o, i, y).wait_send()

    def drain(i, carry):
        for dest in range(nz):
            @pl.when(z < dest)
            def _():
                right_hop(dest, i).wait_send()

            @pl.when(z > dest)
            def _():
                left_hop(dest, i).wait_send()
        return carry

    lax.fori_loop(0, nw, drain, 0)

    for zz in range(nz):
        for o in range(1, ny):
            o_side(zz, o, (y + ny - o) % ny).wait_recv()
            o_side(zz, o, y).wait_send()

        @pl.when(jnp.logical_and(zz <= z, z < nz - 1))
        def _():
            o_right(zz).wait_send()

        @pl.when(jnp.logical_and(zz >= z, z > 0))
        def _():
            o_left(zz).wait_send()


def project(normed, weights, w_out, nz, ny, ntp):
    tokens = normed.shape[0]
    kd, cols = weights[0].shape
    nw = len(weights)
    dma = pltpu.SemaphoreType.DMA
    strip = pltpu.VMEM((nz, nw, tokens, cols), BF16)
    return pl.pallas_call(
        functools.partial(project_kernel, nz, ny, ntp),
        out_shape=(
            jax.ShapeDtypeStruct((nw, tokens, cols), F32),
            jax.ShapeDtypeStruct((nz * ny * w_out.shape[0], w_out.shape[1]), BF16),
        ),
        in_specs=[pl.BlockSpec(memory_space=pltpu.VMEM)] * (2 + nw),
        out_specs=(pl.BlockSpec(memory_space=pltpu.VMEM),) * 2,
        scratch_shapes=[
            pltpu.VMEM((ny, nw, kd, cols), BF16),
            pltpu.VMEM((nz, tokens, ny * kd), BF16),
            strip, strip, strip, strip,
            dma((nw + 2,)),
            dma((ny - 1, nw)), dma((ny - 1, nw)),
            dma((nz - 1,)), dma((nz - 1,)),
            dma((nz - 1, ntp - 1)), dma((nz - 1, ntp - 1)),
            dma((nz, nw)), dma((nz, nw)), dma((nz, nw)), dma((nz, nw)),
            dma((nz,)), dma((nz,)), dma((nz,)), dma((nz,)),
            dma((nz, ny - 1)), dma((nz, ny - 1)),
        ],
        compiler_params=pltpu.CompilerParams(
            collective_id=0, has_side_effects=True, vmem_limit_bytes=27 * 1024 * 1024
        ),
        cost_estimate=pl.CostEstimate(
            flops=2 * tokens * kd * nz * ny * cols * nw, bytes_accessed=300_000_000, transcendentals=0
        ),
    )(normed, *weights, w_out)


def gate_of(pre, bounds):
    return bounds + (1.0 - bounds) * jax.nn.sigmoid(pre.astype(F32))


def split(value):
    high = value.astype(BF16)
    return high, (value - high.astype(F32)).astype(BF16)


def recur_kernel(
    scale, proj_ref, state_ref, pf_ref, pv_ref, acc_ref, bounds_ref, gain_ref,
    head_ref, taken_ref, keys, vals, asks, outs, flat,
):
    steps = pf_ref.shape[0]
    block = state_ref.shape[0]
    bounds = bounds_ref[...]
    accepted = acc_ref[...]

    decay = jnp.ones((block, bounds.shape[-1]), F32)
    for p in reversed(range(steps)):
        gate = gate_of(pf_ref[p], bounds)
        kept = p < accepted
        high, low = split(jnp.where(kept, (1.0 - gate) * decay, 0.0))
        keys[:, p, :] = high.astype(F32)
        keys[:, steps + p, :] = low.astype(F32)
        past = pv_ref[p].astype(F32)
        vals[:, p, :] = past
        vals[:, steps + p, :] = past
        decay = jnp.where(kept, gate * decay, decay)
    decay_t = decay.T

    query, pre, value, gate_in = (
        [proj_ref[i, pl.ds(p, block, stride=steps), :].astype(BF16).astype(F32) for p in range(steps)] for i in range(4)
    )
    forget = [gate_of(pre[p], bounds) for p in range(steps)]
    inner = []
    reach = None
    for p in range(steps):
        ask = query[p] * scale
        total = None
        for s in reversed(range(p + 1)):
            weight = jnp.sum(ask * (1.0 - forget[s]), axis=-1, keepdims=True) * value[s]
            total = weight if total is None else total + weight
            ask = ask * forget[s]
        inner.append(total)
        high, low = split(ask)
        asks[:, p, :] = high.astype(F32)
        asks[:, steps + p, :] = low.astype(F32)

    for s in range(block):
        added = lax.dot_general(
            keys[s].astype(BF16), vals[s].astype(BF16), (((0,), (0,)), ((), ())),
            preferred_element_type=F32,
        )
        taken = decay_t[:, s:s + 1] * state_ref[s, 0] + added
        taken_ref[s, 0] = taken
        outs[s] = jnp.dot(asks[s].astype(BF16), taken.astype(BF16), preferred_element_type=F32)

    for p in range(steps):
        result = outs[:, p, :] + outs[:, steps + p, :] + inner[p]
        scaled = result * lax.rsqrt(jnp.mean(result * result, axis=-1, keepdims=True) + EPSILON)
        gated = gate_in[p]
        flat[pl.ds(p, block, stride=steps), :] = scaled * gain_ref[...] * (gated * jax.nn.sigmoid(gated))
    head_ref[...] = flat[...].astype(BF16)


def recur(proj, state, pf, pv, accepted, bounds, gain):
    seqs, heads, kdim, vdim = state.shape
    steps = pf.shape[0]
    block = min(32, seqs)
    small = lambda: pl.BlockSpec((steps, block, kdim), lambda b, h: (0, b, h))
    row = lambda: pl.BlockSpec((1, kdim), lambda b, h: (0, h))
    body = pltpu.VMEM((block, 2 * steps, kdim), F32)
    return pl.pallas_call(
        functools.partial(recur_kernel, kdim ** (-0.5)),
        grid=(seqs // block, heads),
        out_shape=(
            jax.ShapeDtypeStruct((steps * seqs, heads * vdim), BF16),
            jax.ShapeDtypeStruct(state.shape, F32),
        ),
        in_specs=[
            pl.BlockSpec((4, steps * block, kdim), lambda b, h: (0, b, h)),
            pl.BlockSpec((block, 1, kdim, vdim), lambda b, h: (b, h, 0, 0)),
            small(), small(),
            pl.BlockSpec((block, 1), lambda b, h: (b, 0)),
            row(), row(),
        ],
        out_specs=(
            pl.BlockSpec((steps * block, vdim), lambda b, h: (b, h)),
            pl.BlockSpec((block, 1, kdim, vdim), lambda b, h: (b, h, 0, 0)),
        ),
        scratch_shapes=[body, body, body, body, pltpu.VMEM((steps * block, vdim), F32)],
        compiler_params=pltpu.CompilerParams(
            dimension_semantics=("arbitrary", "arbitrary"), vmem_limit_bytes=14 * 1024 * 1024
        ),
        cost_estimate=pl.CostEstimate(
            flops=4 * state.size, bytes_accessed=8 * state.size, transcendentals=0
        ),
    )(proj, state, pf, pv, accepted, bounds, gain)


def combine_kernel(ntp, head_ref, w_ref, mixed_ref, landed, total, sends, recvs):
    kv = lax.axis_index("kv")
    t = lax.axis_index("tp")
    cols = head_ref.shape[1]
    barrier = pltpu.get_barrier_semaphore()
    for q in range(1, ntp):
        pl.semaphore_signal(barrier, inc=1, device_id=(kv, (t + q) % ntp), device_id_type=MESH)
    pl.semaphore_wait(barrier, ntp - 1)

    def copy(q):
        return pltpu.make_async_remote_copy(
            src_ref=head_ref, dst_ref=landed.at[q - 1],
            send_sem=sends.at[q - 1], recv_sem=recvs.at[q - 1],
            device_id=(kv, (t + q) % ntp), device_id_type=MESH,
        )

    def part(source):
        return w_ref[pl.ds(pl.multiple_of(source * cols, cols), cols), :]

    for q in range(1, ntp):
        copy(q).start()
    total[...] = jnp.dot(head_ref[...], part(t), preferred_element_type=F32)
    for q in range(1, ntp):
        copy(q).wait_recv()
        total[...] += jnp.dot(landed[q - 1], part((t + ntp - q) % ntp), preferred_element_type=F32)
    mixed_ref[...] = total[...].astype(BF16)
    for q in range(1, ntp):
        copy(q).wait_send()


def combine(head, w_all, ntp):
    count, cols = head.shape
    width = w_all.shape[1]
    dma = pltpu.SemaphoreType.DMA
    return pl.pallas_call(
        functools.partial(combine_kernel, ntp),
        out_shape=jax.ShapeDtypeStruct((count, width), BF16),
        in_specs=[pl.BlockSpec(memory_space=pltpu.VMEM)] * 2,
        out_specs=pl.BlockSpec(memory_space=pltpu.VMEM),
        scratch_shapes=[
            pltpu.VMEM((ntp - 1, count, cols), BF16),
            pltpu.VMEM((count, width), F32),
            dma((ntp - 1,)), dma((ntp - 1,)),
        ],
        compiler_params=pltpu.CompilerParams(
            collective_id=1, has_side_effects=True, vmem_limit_bytes=12 * 1024 * 1024
        ),
        cost_estimate=pl.CostEstimate(
            flops=2 * w_all.size * count, bytes_accessed=40_000_000, transcendentals=0
        ),
    )(head, w_all)


def on_device(
    nz, ny, ntp,
    tokens, norm_gain, w_query, w_forget, w_value, w_gate, lower_bound, head_gain,
    w_out, state, prev_forget, prev_value, accepted,
):
    seqs = state.shape[0]
    floated = tokens.astype(F32)
    normed = (
        floated
        * lax.rsqrt(jnp.mean(floated * floated, axis=-1, keepdims=True) + EPSILON)
        * norm_gain
    ).astype(BF16)
    proj, w_all = project(normed, (w_query, w_forget, w_value, w_gate), w_out, nz, ny, ntp)
    cols = proj.shape[-1]
    head_out, taken = recur(
        proj,
        state,
        prev_forget.transpose(1, 0, 2),
        prev_value.transpose(1, 0, 2),
        accepted.reshape(seqs, 1),
        lower_bound.reshape(1, cols),
        head_gain.reshape(1, cols),
    )
    mixed = combine(head_out, w_all, ntp)
    return mixed, taken


def solution(mesh):
    nkv, ntp = mesh.shape["kv"], mesh.shape["tp"]
    ny = max(d for d in range(1, nkv + 1) if nkv % d == 0 and d * d <= nkv)
    return jax.shard_map(
        functools.partial(on_device, nkv // ny, ny, ntp),
        mesh=mesh,
        in_specs=(
            P("kv", None),
            P(),
            P("kv", "tp"),
            P("kv", "tp"),
            P("kv", "tp"),
            P("kv", "tp"),
            P("tp"),
            P("tp"),
            P("kv", "tp"),
            P("kv", "tp", None, None),
            P("kv", None, "tp"),
            P("kv", None, "tp"),
            P("kv"),
        ),
        out_specs=(P("kv", "tp"), P("kv", "tp", None, None)),
        check_vma=False,
    )
```
